512 devices in a mesh: sp: 32 (over z, core), tp: 16 (over y, x).
Axes of the slice: x: 4, y: 4, z: 16, core: 2. Of those that a mesh axis runs over, the one named last changes fastest.
Arguments:
- query_proj: bfloat16 [8192, 2048], P('sp', 'tp'), may hold values from -4 to 4
- key_proj: bfloat16 [8192, 1024], P('sp', 'tp'), may hold values from -4 to 4
- value_proj: bfloat16 [8192, 1024], P('sp', 'tp'), may hold values from -48 to 48
- query_gain: float32 [32, 64], P('tp'), may hold values from 1 to 6
- key_gain: float32 [16, 64], P('tp'), may hold values from 1 to 6
- residual: bfloat16 [8192, 2048], P('sp', 'tp'), may hold values from -48 to 48
- out_weight: bfloat16 [2048, 2048], P(None, 'tp'), may hold values from -0.125 to 0.125
- route_expert: int32 [8192, 8], P('sp'), may hold values from 0 to 255, all different within a row; in each aligned block of 256 rows (0 to 255, 256 to 511, ...) at most 12 rows name the same one
- route_weight: float32 [8192, 8], P('sp'), may hold values from 0.25 to 1.25
- expert_gate: bfloat16 [512, 2048, 256], P(('sp', 'tp')), may hold values from -0.125 to 0.125
- expert_up: bfloat16 [512, 2048, 256], P(('sp', 'tp')), may hold values from -0.125 to 0.125
- expert_down: bfloat16 [512, 256, 2048], P(('sp', 'tp')), may hold values from -0.25 to 0.25
Outputs:
- block_out: bfloat16 [8192, 2048], P('sp', 'tp')
The draws below stay inside these ranges and needn't reach their ends.
Inputs may be any that keep to these rules, and one draw needn't show every extreme that they name: `route_expert`: A row names 8 different experts; among the rows of one index of sp no expert is named by more than 12 rows, a bound that some block reaches of them.
All inputs are finite; a program needn't handle non-finite values.
Results may differ from the reference program's by a relative error of at most 0.012.
The reference program's roundings to bfloat16 on the way count: a program that leaves them out, or rounds other values in their place, can miss the bound.
Values may be sent and summed in bfloat16 or wider, within the bound.
A program may use at most 64 MiB of HBM per device.

```python
import math
import jax
import jax.numpy as jnp
import numpy as np
from jax import lax

D = 2048
HEADS = 32
KV_HEADS = 16
HEAD_DIM = 64
FF = 512
TOP_K = 8
GRID_W = 64
TOK_DEV = 256
TOKENS = 8192
EXPERTS = 256
CAP = 12
N_SP = 32


def attention_pair(key):
    seeded = jax.random.fold_in(key, 11)
    first_key, second_key = jax.random.split(seeded, 2)
    key_rows = jnp.clip(jax.random.normal(first_key, (TOKENS, KV_HEADS, HEAD_DIM), jnp.float32), -4.0, 4.0)
    query_rows = jnp.clip(jax.random.normal(second_key, (TOKENS, HEADS, HEAD_DIM), jnp.float32), -4.0, 4.0)
    return (query_rows.reshape(TOKENS, HEADS * HEAD_DIM), key_rows.reshape(TOKENS, KV_HEADS * HEAD_DIM))


def draw_query_proj(key, part):
    return attention_pair(key)[0].astype(jnp.bfloat16)


def draw_key_proj(key, part):
    return attention_pair(key)[1].astype(jnp.bfloat16)


def draw_query_gain(key, part):
    seeded = jax.random.fold_in(key, 31)
    return jnp.exp(jax.random.uniform(seeded, (HEADS, HEAD_DIM), jnp.float32, 0.0, 0.6931))


def draw_key_gain(key, part):
    seeded = jax.random.fold_in(key, 37)
    return jnp.exp(jax.random.uniform(seeded, (KV_HEADS, HEAD_DIM), jnp.float32, 0.0, 0.6931))


def draw_residual(key, part):
    seeded = jax.random.fold_in(key, 41)
    first_key, second_key = jax.random.split(seeded, 2)
    fraction = jnp.arange(D, dtype=jnp.float32) / D
    row_scale = jnp.exp(jax.random.uniform(second_key, (TOKENS, 1), jnp.float32, -0.6931, 1.6094))
    column_scale = 0.6 * 3.0 ** fraction
    pattern = jnp.clip(jax.random.normal(first_key, (TOKENS, D), jnp.float32), -4.0, 4.0)
    return (pattern * row_scale * column_scale[None, :]).astype(jnp.bfloat16)


def block_scale(rng, extent, pieces, low, top_value):
    def one(dim, shards_of):
        steps = jax.random.uniform(jax.random.fold_in(jax.random.fold_in(rng, 6), dim), (shards_of,), jnp.float32, low / len(pieces), top_value / len(pieces))
        return jnp.repeat(jnp.exp(steps), extent[dim] // shards_of).reshape((-1,) + (1,) * (len(extent) - dim - 1))

    factor_of = one(*pieces[0])
    for cut in pieces[1:]:
        factor_of = factor_of * one(*cut)
    return factor_of


def assign_block(key, own, number, rows, amount, top, most, skew):
    ranking = jax.random.permutation(key, amount)
    crowded, usual = shares(amount, rows * top, most, skew, True), shares(amount, rows * top, most, skew, False)
    places = jnp.arange(amount)

    def named(sizes, turn):
        used = int((sizes > 0).sum())
        fixed = max(1, used // 4)
        passed = fixed + (places - fixed + turn * (used - fixed)) % max(1, amount - fixed)
        return jnp.zeros((amount,), jnp.int32).at[ranking[jnp.where(places < fixed, places, passed)]].set(jnp.asarray(sizes, jnp.int32))

    sizes = jnp.where(number % 4 == 0, named(crowded, number // 4), named(usual, number - number // 4 - 1))
    mixed = jax.random.permutation(jax.random.fold_in(own, 3), amount)
    giver, receiver = mixed[0:amount // 2 * 2:2], mixed[1:amount // 2 * 2:2]
    margin = jnp.minimum(sizes[giver] - 1, most - sizes[receiver]) // 2
    margin = jnp.where((giver == ranking[0]) | (receiver == ranking[0]) | (sizes[receiver] == 0), 0, jnp.maximum(margin, 0))
    passed = jax.random.randint(jax.random.fold_in(own, 4), (amount // 2,), 0, 1 << 20) % (margin + 1)
    sizes = sizes.at[giver].add(-passed).at[receiver].add(passed)
    labels = jnp.searchsorted(jnp.cumsum(sizes), jnp.arange(rows * top), side="right").astype(jnp.int32)
    grid = labels.reshape(top, rows).T
    grid = grid[jax.random.permutation(jax.random.fold_in(own, 1), rows)]
    turn = jax.random.randint(jax.random.fold_in(own, 2), (rows, 1), 0, top)
    return jnp.take_along_axis(grid, (jnp.arange(top)[None, :] + turn) % top, axis=1)


def shares(count, total, limit, skew, full):
    weights = [(1 << 20) // math.isqrt(grade ** skew) + 1 for grade in range(1, count + 1)]
    largest = limit if full else min(limit, max(-(-total // count), total * weights[0] // sum(weights)))
    least = 1 if total - largest >= count - 1 else 0
    holding, spare = [largest] + [least] * (count - 1), total - largest - least * (count - 1)
    while spare > 0:
        movable = [i for i in range(1, count) if holding[i] < largest] or [i for i in range(1, count) if holding[i] < limit]
        pool, remaining = sum([weights[i] for i in movable]), spare
        for i in movable:
            more = min(limit - holding[i], max(1, remaining * weights[i] // pool), spare)
            holding[i] = holding[i] + more
            spare = spare - more
    return np.array(holding)


def centred(own_key, shape, deviation, most, cuts=(), kind=jnp.bfloat16):
    level = block_scale(own_key, shape, cuts, -0.22, 0.18) if cuts else 1.0
    entries = jax.random.normal(own_key, shape, jnp.float32) * deviation * level
    return jnp.minimum(jnp.maximum(entries, -most), most).astype(kind)


def setup_inputs(seed: int = 0) -> dict:
    key_of = jax.random.split(jax.random.key(seed), 13)
    query_proj = draw_query_proj(jax.random.fold_in(key_of[12], 71), 0)
    key_proj = draw_key_proj(jax.random.fold_in(key_of[12], 71), 0)
    value_proj = centred(key_of[2], (TOKENS, KV_HEADS * HEAD_DIM), 8.0, 48.0, ((0, 32), (1, 16)))
    query_gain = draw_query_gain(jax.random.fold_in(key_of[12], 71), 0)
    key_gain = draw_key_gain(jax.random.fold_in(key_of[12], 71), 0)
    residual = draw_residual(jax.random.fold_in(key_of[12], 71), 0)
    out_weight = centred(key_of[6], (HEADS * HEAD_DIM, D), (HEADS * HEAD_DIM) ** -0.5, 0.125, ((1, 16),))
    route_expert_keys = jax.random.split(jax.random.fold_in(key_of[7], 1), TOKENS // TOK_DEV)
    route_expert_turns = jax.random.permutation(jax.random.fold_in(key_of[7], 3), TOKENS // TOK_DEV)
    route_expert = jax.vmap(lambda own, number: assign_block(jax.random.fold_in(key_of[7], 2), own, number, TOK_DEV, EXPERTS, TOP_K, CAP, 1))(route_expert_keys, route_expert_turns).reshape((TOKENS, TOP_K))
    route_weight = jnp.clip(0.25 + 1.0 * jax.random.uniform(key_of[8], (TOKENS, TOP_K), jnp.float32) ** block_scale(key_of[8], (TOKENS, TOP_K), ((0, 32),), -0.2, 0.2), 0.25, 1.25)
    expert_gate = centred(key_of[9], (2 * EXPERTS, D, FF // 2), D ** -0.5, 0.125, ((0, 512),))
    expert_up = centred(key_of[10], (2 * EXPERTS, D, FF // 2), D ** -0.5, 0.125, ((0, 512),))
    expert_down = centred(key_of[11], (2 * EXPERTS, FF // 2, D), FF ** -0.5, 0.25, ((0, 512),))
    return dict(query_proj=query_proj, key_proj=key_proj, value_proj=value_proj, query_gain=query_gain, key_gain=key_gain, residual=residual, out_weight=out_weight, route_expert=route_expert, route_weight=route_weight, expert_gate=expert_gate, expert_up=expert_up, expert_down=expert_down)


EPSILON = 1e-06
ROPE_BASE = 10000.0

def rotation_tables(offset, count):
    pair_count = HEAD_DIM // 4
    position = offset + jnp.arange(count, dtype=jnp.int32)
    grid_row = (position // GRID_W).astype(jnp.float32)
    grid_col = (position % GRID_W).astype(jnp.float32)
    inverse = ROPE_BASE ** (-jnp.arange(pair_count, dtype=jnp.float32) / pair_count)
    angles = jnp.stack([grid_row[:, None] * inverse, grid_col[:, None] * inverse], axis=1)
    return (jnp.cos(angles), jnp.sin(angles))

def rotate(vectors, cosine_table, sine_table):
    pair_count = HEAD_DIM // 4
    shaped = vectors.reshape(vectors.shape[:-1] + (2, 2, pair_count))
    first_half = shaped[..., 0, :]
    second_half = shaped[..., 1, :]
    cosine_row = cosine_table[:, None]
    sine_row = sine_table[:, None]
    turned = jnp.stack([first_half * cosine_row - second_half * sine_row, first_half * sine_row + second_half * cosine_row], axis=-2)
    return turned.reshape(vectors.shape)

def head_norm(vectors, gain):
    scaled = vectors.astype(jnp.float32)
    scaled = scaled * lax.rsqrt(lax.optimization_barrier(jnp.mean(scaled * scaled, axis=-1, keepdims=True)) + EPSILON)
    return scaled * gain.astype(jnp.float32)

def slot_layout(choices, weights):
    token_count = choices.shape[0]
    flat_choice = choices.reshape(token_count * TOP_K).astype(jnp.int32)
    onehot = (flat_choice[:, None] == jnp.arange(EXPERTS, dtype=jnp.int32)[None, :]).astype(jnp.int32)
    earlier = jnp.cumsum(onehot, axis=0) - onehot
    slot_rank = lax.optimization_barrier(jnp.sum(earlier * onehot, axis=1))
    position = (flat_choice * CAP + slot_rank).astype(jnp.int32)
    owner = (jnp.arange(token_count * TOP_K, dtype=jnp.int32) // TOP_K).astype(jnp.int32)
    slot_token = jnp.full((EXPERTS * CAP,), token_count, jnp.int32).at[position].set(owner)
    slot_weight = jnp.zeros((EXPERTS * CAP,), jnp.float32).at[position].set(weights.reshape(token_count * TOP_K).astype(jnp.float32))
    return (slot_token, slot_weight)

def reference(query_proj, key_proj, value_proj, query_gain, key_gain, residual, out_weight, route_expert, route_weight, expert_gate, expert_up, expert_down):
    token_total = query_proj.shape[0]
    group_size = HEADS // KV_HEADS
    cosine_table, sine_table = rotation_tables(0, token_total)
    query_rot = rotate(head_norm(query_proj.reshape(token_total, HEADS, HEAD_DIM), query_gain), cosine_table, sine_table).astype(jnp.bfloat16)
    key_rot = rotate(head_norm(key_proj.reshape(token_total, KV_HEADS, HEAD_DIM), key_gain), cosine_table, sine_table).astype(jnp.bfloat16)
    value_heads = value_proj.reshape(token_total, KV_HEADS, HEAD_DIM)
    block_len = math.gcd(token_total, 1024)

    def one_head(head_index):
        query_head = lax.dynamic_index_in_dim(query_rot, head_index, 1, keepdims=False)
        key_head = lax.dynamic_index_in_dim(key_rot, head_index // group_size, 1, keepdims=False)
        value_head = lax.dynamic_index_in_dim(value_heads, head_index // group_size, 1, keepdims=False)
        query_blocks = query_head.reshape(token_total // block_len, block_len, HEAD_DIM)

        def one_block(query_block):
            scores = jnp.dot(query_block, key_head.T, preferred_element_type=jnp.float32) * HEAD_DIM ** (-0.5)
            weights = jnp.exp(scores - lax.optimization_barrier(jnp.max(scores, axis=-1, keepdims=True))).astype(jnp.bfloat16)
            weight_sum = lax.optimization_barrier(jnp.sum(weights.astype(jnp.float32), axis=-1, keepdims=True))
            summed = jnp.dot(weights, value_head, preferred_element_type=jnp.float32)
            return (summed / weight_sum).astype(jnp.bfloat16)
        return lax.map(one_block, query_blocks).reshape(token_total, HEAD_DIM)
    attended = lax.map(one_head, jnp.arange(HEADS, dtype=jnp.int32))
    attended = jnp.transpose(attended, (1, 0, 2)).reshape(token_total, HEADS * HEAD_DIM)
    mixed_sum = residual.astype(jnp.float32) + jnp.dot(attended, out_weight, preferred_element_type=jnp.float32)
    mixed_rows = mixed_sum.astype(jnp.bfloat16)
    slot_token, slot_weight = jax.vmap(slot_layout)(route_expert.reshape(N_SP, TOK_DEV, TOP_K), route_weight.reshape(N_SP, TOK_DEV, TOP_K))
    source_base = (jnp.arange(N_SP, dtype=jnp.int32) * TOK_DEV)[:, None]
    global_index = jnp.where(slot_token == TOK_DEV, token_total, slot_token + source_base).astype(jnp.int32)
    grouped_rows = mixed_rows.reshape(N_SP, TOK_DEV, D)
    padded_rows = jnp.concatenate([grouped_rows, jnp.zeros((N_SP, 1, D), jnp.bfloat16)], axis=1)

    def one_expert(routed, expert_index):
        token_ids = lax.dynamic_slice_in_dim(slot_token, expert_index * CAP, CAP, 1)
        expert_rows = jax.vmap(lambda table, index: table[index])(padded_rows, token_ids).reshape(N_SP * CAP, D)
        squares = lax.optimization_barrier(jnp.mean(jnp.square(expert_rows.astype(jnp.float32)), axis=-1, keepdims=True))
        norm_scale = lax.rsqrt(squares + EPSILON)
        total = jnp.zeros((N_SP * CAP, D), jnp.float32)
        for half in range(2):
            block = 2 * expert_index + half
            gate_value = jnp.dot(expert_rows, lax.dynamic_index_in_dim(expert_gate, block, 0, keepdims=False), preferred_element_type=jnp.float32) * norm_scale
            up_value = jnp.dot(expert_rows, lax.dynamic_index_in_dim(expert_up, block, 0, keepdims=False), preferred_element_type=jnp.float32) * norm_scale
            hidden = (jax.nn.silu(gate_value) * up_value).astype(jnp.bfloat16)
            produced = jnp.dot(hidden, lax.dynamic_index_in_dim(expert_down, block, 0, keepdims=False), preferred_element_type=jnp.float32).astype(jnp.bfloat16)
            total = total + lax.optimization_barrier(produced).astype(jnp.float32)
        slot_weights = lax.dynamic_slice_in_dim(slot_weight, expert_index * CAP, CAP, 1).reshape(N_SP * CAP)
        targets = lax.dynamic_slice_in_dim(global_index, expert_index * CAP, CAP, 1).reshape(N_SP * CAP)
        routed = routed.at[targets].add(total * slot_weights[:, None])
        return (routed, None)
    routed, unused = lax.scan(one_expert, jnp.zeros((token_total + 1, D), jnp.float32), jnp.arange(EXPERTS, dtype=jnp.int32))
    return (mixed_sum + routed[:token_total]).astype(jnp.bfloat16)
```

```python
import functools

import jax
import jax.numpy as jnp
import numpy as np
from jax import lax
from jax.experimental import pallas as pl
from jax.experimental.pallas import tpu as pltpu
from jax.sharding import Mesh
from jax.sharding import PartitionSpec as P

EPS = 1e-06
CAP = 12
TOK = 256
HALF = 128
LANES = 128
GROUP = 4 * CAP
F32 = jnp.float32
BF16 = jnp.bfloat16
MESH = pl.DeviceIdType.MESH
SP = ("z", "c")
TP = ("y", "x")
ALL = ("z", "c", "y", "x")


def rotation_constants(rows):
    pairs = 16
    inverse = np.float32(10000.0) ** (-np.arange(pairs, dtype=np.float32) / np.float32(pairs))
    inverse = inverse.astype(np.float32)
    lane = np.arange(LANES)
    freq = inverse[lane % 16]
    sign = np.where((lane // 16) % 2 == 0, -1.0, 1.0)

    def table(count):
        angle = (np.arange(count, dtype=np.float32)[:, None] * freq[None, :]).astype(np.float32)
        angle = angle.astype(np.float64)
        return np.stack([np.cos(angle), np.sin(angle) * sign[None, :]]).astype(np.float32)

    return table(rows), table(64)


def places():
    return lax.axis_index("z"), lax.axis_index("c"), lax.axis_index("y"), lax.axis_index("x")


def plane_id(place, nx):
    return {"y": place // nx, "x": place % nx}


def barrier_all(z, c, me, nz, ntp, nx):
    barrier = pltpu.get_barrier_semaphore()

    def one(d, carry):
        t = (me + d) % ntp
        pl.semaphore_signal(barrier, inc=1, device_id=plane_id(t, nx), device_id_type=MESH)
        return carry

    lax.fori_loop(1, ntp, one, 0)
    pl.semaphore_signal(barrier, inc=1, device_id={"z": (z + 1) % nz}, device_id_type=MESH)
    pl.semaphore_signal(barrier, inc=1, device_id={"z": (z + nz - 1) % nz}, device_id_type=MESH)
    pl.semaphore_signal(barrier, inc=1, device_id={"c": 1 - c}, device_id_type=MESH)
    pl.semaphore_wait(barrier, ntp - 1 + 3)


def wait_bytes(ref, sem):
    pltpu.make_async_copy(ref, ref, sem).wait()


class Ring:
    def __init__(self, buf, z, c, nz, send_sem, recv_sem, pair_sem):
        self.buf, self.z, self.c, self.nz = buf, z, c, nz
        self.h = nz // 2
        self.send_sem, self.recv_sem, self.pair_sem = send_sem, recv_sem, pair_sem

    def piece(self, chip, core, sub):
        return self.buf.at[chip * 2 + core, pl.ds(sub * HALF, HALF)]

    def hop(self, chip, direction, sub, step):
        to = (self.z + (1 if direction == 0 else self.nz - 1)) % self.nz
        part = self.piece(chip, self.c, sub)
        return pltpu.make_async_remote_copy(
            src_ref=part,
            dst_ref=part,
            send_sem=self.send_sem,
            recv_sem=self.recv_sem.at[direction, sub, step],
            device_id={"z": to},
            device_id_type=MESH,
        )

    def pair(self, chip, sub, order):
        part = self.piece(chip, self.c, sub)
        return pltpu.make_async_remote_copy(
            src_ref=part,
            dst_ref=part,
            send_sem=self.send_sem,
            recv_sem=self.pair_sem.at[order, sub],
            device_id={"c": 1 - self.c},
            device_id_type=MESH,
        )

    def begin(self):
        for sub in range(2):
            for direction in range(2):
                self.hop(self.z, direction, sub, 1).start()
        for sub in range(2):
            self.pair(self.z, sub, 0).start()

    def step(self, s):
        h, nz = self.h, self.nz
        for sub in range(2):
            for direction in range(2):
                chip = (self.z + (nz - s if direction == 0 else s)) % nz
                order = jnp.minimum(2 * s - 1 + direction, 2 * h - 1)
                last = h if direction == sub else h - 1

                @pl.when(s <= last)
                def _():
                    wait_bytes(self.piece(chip, self.c, sub), self.recv_sem.at[direction, sub, s])

                @pl.when(s < last)
                def _():
                    self.hop(chip, direction, sub, s + 1).start()

                @pl.when(s <= last)
                def _():
                    self.pair(chip, sub, order).start()

    def wait_pair(self, chip, order):
        for sub in range(2):
            wait_bytes(self.piece(chip, 1 - self.c, sub), self.pair_sem.at[order, sub])

    def finish(self):
        wait_bytes(self.buf.at[pl.ds(0, 2 * self.nz - 1)], self.send_sem)


def attention_kernel(
    dims,
    q_ref, k_ref, v_ref, qg_ref, kg_ref, res_ref, ow_ref, route_ref, rowtab_ref, coltab_ref,
    mixed_ref, routes_ref,
    kvbuf, rbuf, qz, run_max, run_sum, acc, attsend, attbuf,
    ring_send, ring_recv, ring_pair, route_send, route_recv, route_pair, att_send, att_recv,
):
    nz, ny, nx = dims
    ntp = ny * nx
    h = nz // 2
    z, c, y, x = places()
    me = y * nx + x
    sp = z * 2 + c
    ring = Ring(kvbuf, z, c, nz, ring_send, ring_recv, ring_pair)

    lane = lax.broadcasted_iota(jnp.int32, (64, LANES), 1)
    low = lane < 64
    even = (lane // 16) % 2 == 0
    row_half = (lane % 64) < 32

    def normed(values, gain, both):
        squares = values * values
        first = jnp.sum(jnp.where(low, squares, 0.0), axis=1, keepdims=True) / 64.0
        scale = lax.rsqrt(first + EPS)
        if both:
            second = jnp.sum(jnp.where(low, 0.0, squares), axis=1, keepdims=True) / 64.0
            scale = jnp.where(low, scale, lax.rsqrt(second + EPS))
        return values * scale * gain

    def turned(values, cosine, sine):
        partner = jnp.where(even, pltpu.roll(values, 112, 1), pltpu.roll(values, 16, 1))
        return values * cosine + partner * sine

    kgain = jnp.concatenate([kg_ref[...], kg_ref[...]], axis=1)
    qgain = jnp.concatenate([qg_ref[0:1, :], qg_ref[1:2, :]], axis=1)
    for part in range(4):
        rows = slice(part * 64, part * 64 + 64)
        row = sp * 4 + part
        cosine = jnp.where(row_half, rowtab_ref[0, pl.ds(row, 1), :], coltab_ref[0])
        sine = jnp.where(row_half, rowtab_ref[1, pl.ds(row, 1), :], coltab_ref[1])
        packed = jnp.concatenate([k_ref[rows, :], v_ref[rows, :]], axis=1).astype(F32)
        keys = turned(normed(packed, kgain, False), cosine, sine)
        kvbuf[sp, rows, :] = jnp.where(low, keys, packed).astype(BF16)
        query = turned(normed(q_ref[rows, :].astype(F32), qgain, True), cosine, sine)
        query = query.astype(BF16).astype(F32) * 0.125
        qz[rows, :] = jnp.where(low, query, 0.0).astype(BF16)
        qz[slice(TOK + part * 64, TOK + part * 64 + 64), :] = jnp.where(
            low, pltpu.roll(query, 64, 1), 0.0
        ).astype(BF16)
    rbuf[sp] = route_ref[...]
    run_max[...] = jnp.full((1, 2 * TOK), -1e30, F32)
    run_sum[...] = jnp.zeros((1, 2 * TOK), F32)
    acc[...] = jnp.zeros((LANES, 2 * TOK), F32)

    barrier_all(z, c, me, nz, ntp, nx)
    ring.begin()

    def route_hop(chip, direction, step):
        to = (z + (1 if direction == 0 else nz - 1)) % nz
        part = rbuf.at[chip * 2 + c]
        return pltpu.make_async_remote_copy(
            src_ref=part, dst_ref=part, send_sem=route_send,
            recv_sem=route_recv.at[direction, step],
            device_id={"z": to}, device_id_type=MESH,
        )

    def route_cross(chip, order):
        part = rbuf.at[chip * 2 + c]
        return pltpu.make_async_remote_copy(
            src_ref=part, dst_ref=part, send_sem=route_send,
            recv_sem=route_pair.at[order],
            device_id={"c": 1 - c}, device_id_type=MESH,
        )

    for direction in range(2):
        route_hop(z, direction, 1).start()
    route_cross(z, 0).start()

    def update(u, carry):
        g = (u + 1) // 2
        chip = (z + nz + (1 - 2 * (u % 2)) * g) % nz
        ring.wait_pair(chip, u)
        block = kvbuf[pl.ds(chip * 2, 2)].reshape(2 * TOK, LANES)
        scores = lax.dot_general(
            block, qz[...], (((1,), (1,)), ((), ())), preferred_element_type=F32
        )
        old = run_max[...]
        new = jnp.maximum(old, jnp.max(scores, axis=0, keepdims=True))
        weights = jnp.exp(scores - new).astype(BF16)
        rescale = jnp.exp(old - new)
        run_max[...] = new
        run_sum[...] = run_sum[...] * rescale + jnp.sum(
            weights.astype(F32), axis=0, keepdims=True
        )
        acc[...] = acc[...] * rescale + lax.dot_general(
            block, weights, (((0,), (0,)), ((), ())), preferred_element_type=F32
        )
        return carry

    def step(s, carry):
        @pl.when(s <= h)
        def _():
            ring.step(s)
            for direction in range(2):
                chip = (z + (nz - s if direction == 0 else s)) % nz
                last = h - direction

                @pl.when(s <= last)
                def _():
                    wait_bytes(rbuf.at[chip * 2 + c], route_recv.at[direction, s])

                @pl.when(s < last)
                def _():
                    route_hop(chip, direction, s + 1).start()

                @pl.when(s <= last)
                def _():
                    route_cross(chip, 2 * s - 1 + direction).start()

        lax.fori_loop(jnp.maximum(2 * s - 3, 0), jnp.minimum(2 * s - 1, 2 * h), update, 0)
        return carry

    lax.fori_loop(1, h + 2, step, 0)

    value = acc[64:128, :] / run_sum[...]
    stacked = jnp.concatenate([value[:, 0:TOK], value[:, TOK : 2 * TOK]], axis=0)
    attended = stacked.T.astype(BF16)
    attsend[...] = attended
    mine = pl.ds(pl.multiple_of(me * LANES, LANES), LANES)
    attbuf[:, mine] = attended

    def spread(d, carry):
        t = (me + d) % ntp
        pltpu.make_async_remote_copy(
            src_ref=attsend, dst_ref=attbuf.at[:, mine], send_sem=att_send, recv_sem=att_recv,
            device_id=plane_id(t, nx), device_id_type=MESH,
        ).start()
        return carry

    lax.fori_loop(1, ntp, spread, 0)

    def route_wait(u, carry):
        g = (u + 1) // 2
        chip = (z + nz + (1 - 2 * (u % 2)) * g) % nz
        wait_bytes(rbuf.at[chip * 2 + 1 - c], route_pair.at[u])
        return carry

    lax.fori_loop(0, 2 * h, route_wait, 0)
    routes_ref[...] = rbuf[...]
    ring.finish()
    wait_bytes(rbuf.at[pl.ds(0, 2 * nz - 1)], route_send)
    pieces = kvbuf.at[pl.ds(0, ntp - 1)]
    wait_bytes(pieces, att_recv)
    mixed_ref[...] = res_ref[...].astype(F32) + jnp.dot(
        attbuf[...], ow_ref[...], preferred_element_type=F32
    )
    wait_bytes(pieces, att_send)


def expert_kernel(
    dims,
    mixed_ref, routes_ref, gate_ref, up_ref, down_ref,
    out_ref,
    rowbuf, marks, keyb, wb, sbuf, wrow, sendd, xbuf, wg, wu, wd, rsend, ret,
    keep, psend, prs, rss, rsr,
    ring_send, ring_recv, ring_pair, disp_send, disp_recv, disp_own, weight_sem,
    ret_send, ret_recv, ret_own, pair_send, pair_recv, rs_send, rs_recv,
):
    nz, ny, nx = dims
    ntp = ny * nx
    h = nz // 2
    experts = ntp // 2
    width = ntp * LANES
    z, c, y, x = places()
    me = y * nx + x
    sp = z * 2 + c
    column, half = me // 2, me % 2
    ring = Ring(rowbuf, z, c, nz, ring_send, ring_recv, ring_pair)

    rowbuf[sp] = mixed_ref[...].astype(BF16)
    loads = [
        pltpu.make_async_copy(source.at[0], target, weight_sem.at[i])
        for i, (source, target) in enumerate(((gate_ref, wg), (up_ref, wu), (down_ref, wd)))
    ]
    for load in loads:
        load.start()
    barrier_all(z, c, me, nz, ntp, nx)
    ring.begin()

    number = (sp * experts + lax.broadcasted_iota(jnp.int32, (8, TOK), 0)).astype(F32)

    def mark(b, carry):
        hit = jnp.zeros((8, TOK), F32)
        weight = jnp.zeros((8, TOK), F32)
        for k in range(8):
            same = routes_ref[b, k : k + 1, :] == number
            hit = hit + jnp.where(same, 1.0, 0.0)
            weight = weight + jnp.where(same, routes_ref[b, 8 + k : 9 + k, :], 0.0)
        marks[b] = hit
        wb[b] = weight
        return carry

    lax.fori_loop(0, 2 * nz, mark, 0)
    before = jnp.where(
        lax.broadcasted_iota(jnp.int32, (TOK, TOK), 0)
        < lax.broadcasted_iota(jnp.int32, (TOK, TOK), 1),
        1.0,
        0.0,
    ).astype(BF16)
    flat = marks[...].reshape(2 * nz * 8, TOK)
    rank = jnp.dot(flat.astype(BF16), before, preferred_element_type=F32)
    keyb[...] = jnp.where(flat > 0.5, rank, -1000.0).reshape(2 * nz, 8, TOK)
    slot = lax.broadcasted_iota(jnp.int32, (GROUP, TOK), 0).astype(F32)

    def chips(g):
        return (z + nz - g) % nz, (z + g % h) % nz

    def dispatch(g):
        first, second = chips(g)
        ring.wait_pair(first, 2 * g - 1)
        ring.wait_pair(second, 2 * g % (2 * h))
        total = jnp.zeros((GROUP, TOK), F32)
        for i in range(4):
            b = (first if i < 2 else second) * 2 + i % 2
            key = keyb[b]
            for j in range(experts):
                hit = key[j : j + 1, :] + float(CAP * i) == slot
                sbuf[g - 1, j * GROUP : (j + 1) * GROUP, i * TOK : (i + 1) * TOK] = jnp.where(
                    hit, 1.0, 0.0
                ).astype(BF16)
            own_key = keyb[b, pl.ds(column, 1), :]
            own_weight = wb[b, pl.ds(column, 1), :]
            total = total + jnp.where(own_key + float(CAP * i) == slot, own_weight, 0.0)
        wrow[g - 1] = jnp.broadcast_to(jnp.sum(total, axis=1, keepdims=True), (GROUP, LANES))
        chosen = jnp.dot(
            sbuf[g - 1, :, 0 : 2 * TOK],
            rowbuf[pl.ds(first * 2, 2)].reshape(2 * TOK, LANES),
            preferred_element_type=F32,
        ) + jnp.dot(
            sbuf[g - 1, :, 2 * TOK : 4 * TOK],
            rowbuf[pl.ds(second * 2, 2)].reshape(2 * TOK, LANES),
            preferred_element_type=F32,
        )
        sendd[g - 1] = chosen.astype(BF16).reshape(experts, GROUP, LANES)
        target = xbuf.at[
            pl.ds(pl.multiple_of((g - 1) * GROUP, 16), GROUP),
            pl.ds(pl.multiple_of(me * LANES, LANES), LANES),
        ]

        def one(d, carry):
            t = (me + d) % ntp
            pltpu.make_async_remote_copy(
                src_ref=sendd.at[g - 1, t // 2], dst_ref=target,
                send_sem=disp_send, recv_sem=disp_recv.at[g - 1],
                device_id=plane_id(t, nx), device_id_type=MESH,
            ).start()
            return carry

        lax.fori_loop(1, ntp, one, 0)
        pltpu.make_async_copy(sendd.at[g - 1, column], target, disp_own.at[g - 1]).start()

    pieces = ret.at[pl.ds(0, ntp - 1)]

    def compute(p):
        for k in range(2):
            wait_bytes(pieces, disp_recv.at[2 * p + k])
            wait_bytes(ret.at[0], disp_own.at[2 * p + k])
        rows = xbuf[pl.ds(pl.multiple_of(p * 2 * GROUP, 16), 2 * GROUP), :]
        wide = rows.astype(F32)
        scale = lax.rsqrt(jnp.sum(wide * wide, axis=1, keepdims=True) / float(width) + EPS)
        gate = jnp.dot(rows, wg[...], preferred_element_type=F32) * scale
        up = jnp.dot(rows, wu[...], preferred_element_type=F32) * scale
        hidden = (gate / (1.0 + jnp.exp(-gate)) * up).astype(BF16)
        factor = wrow[pl.ds(2 * p, 2)].reshape(2 * GROUP, LANES)

        def slices(n, carry):
            columns = pl.ds(pl.multiple_of(n * 2 * LANES, 2 * LANES), 2 * LANES)
            result = jnp.dot(hidden, wd[:, columns], preferred_element_type=F32)
            result = result.astype(BF16).astype(F32)
            for k in range(2):
                part = result[:, k * LANES : (k + 1) * LANES] * factor
                rsend[2 * n + k, pl.ds(2 * p, 2)] = part.astype(BF16).reshape(2, GROUP, LANES)
            return carry

        lax.fori_loop(0, ntp // 2, slices, 0)

    early = max(0, (h - 5) // 2 + 1)
    chunks = h // 2

    def step(s, carry):
        @pl.when(s <= h)
        def _():
            ring.step(s)

        @pl.when((s >= 2) & (s <= h + 1))
        def _():
            dispatch(s - 1)

        @pl.when(s == min(5, h + 2))
        def _():
            for load in loads:
                load.wait()

        is_early = (s >= 5) & (s <= h) & ((s + 1) % 2 == 0)

        @pl.when(is_early | (s >= h + 2))
        def _():
            compute(jnp.where(s >= h + 2, early + s - (h + 2), (s - 5) // 2))

        return carry

    lax.fori_loop(1, h + 2 + chunks - early, step, 0)

    def give(i, carry):
        g = h - i
        target = ret.at[(g - 1) * ntp + half * experts + column]

        def one(d, inner):
            t = (me + d) % ntp
            pltpu.make_async_remote_copy(
                src_ref=rsend.at[t, g - 1], dst_ref=target,
                send_sem=ret_send, recv_sem=ret_recv.at[g - 1],
                device_id=plane_id(t, nx), device_id_type=MESH,
            ).start()
            return inner

        lax.fori_loop(1, ntp, one, 0)
        pltpu.make_async_copy(rsend.at[me, g - 1], target, ret_own.at[g - 1]).start()
        return carry

    lax.fori_loop(0, h, give, 0)

    def combine(g):
        wait_bytes(pieces, ret_recv.at[g - 1])
        wait_bytes(ret.at[0], ret_own.at[g - 1])
        blocks = [
            ret[pl.ds((g - 1) * ntp + k * experts, experts)].reshape(experts * GROUP, LANES)
            for k in range(2)
        ]

        def partial(side, core):
            columns = pl.ds(pl.multiple_of(side * 2 * TOK + core * TOK, TOK), TOK)
            chosen = sbuf[g - 1, :, columns]
            return lax.dot_general(
                chosen, blocks[0], (((0,), (0,)), ((), ())), preferred_element_type=F32
            ) + lax.dot_general(
                chosen, blocks[1], (((0,), (0,)), ((), ())), preferred_element_type=F32
            )

        for side in range(2):
            psend[(g - 1) * 2 + side] = partial(side, 1 - c).astype(BF16)
            pltpu.make_async_remote_copy(
                src_ref=psend.at[(g - 1) * 2 + side], dst_ref=prs.at[(g - 1) * 2 + side],
                send_sem=pair_send, recv_sem=pair_recv.at[(g - 1) * 2 + side],
                device_id={"c": 1 - c}, device_id_type=MESH,
            ).start()
        for side in range(2):
            keep[(g - 1) * 2 + side] = partial(side, c)

    def pass_on(r):
        g = h + 1 - r
        for side in range(2):
            wait_bytes(prs.at[(g - 1) * 2 + side], pair_recv.at[(g - 1) * 2 + side])
        for sub in range(2):
            rows = slice(sub * HALF, sub * HALF + HALF)
            for direction in range(2):
                index = (g - 1) * 2 + jnp.where(r == 1, 0, 1 - direction)
                same = direction == sub
                first_send = 1 if same else 2
                first_add = 2 if same else 3
                slot_of = (direction * 2 + sub) * h + r - 1

                @pl.when(r >= first_add)
                def _():
                    wait_bytes(rsr.at[slot_of - 1], rs_recv.at[slot_of - 1])
                    rss[slot_of] = (
                        keep[index, rows, :]
                        + prs[index, rows, :].astype(F32)
                        + rsr[slot_of - 1].astype(F32)
                    ).astype(BF16)

                @pl.when(r == first_send)
                def _():
                    rss[slot_of] = (
                        keep[index, rows, :] + prs[index, rows, :].astype(F32)
                    ).astype(BF16)

                @pl.when(r >= first_send)
                def _():
                    to = (z + (1 if direction == 0 else nz - 1)) % nz
                    pltpu.make_async_remote_copy(
                        src_ref=rss.at[slot_of], dst_ref=rsr.at[slot_of],
                        send_sem=rs_send, recv_sem=rs_recv.at[slot_of],
                        device_id={"z": to}, device_id_type=MESH,
                    ).start()

    def back(s, carry):
        @pl.when(s <= h)
        def _():
            combine(h + 1 - s)

        @pl.when(s >= 2)
        def _():
            pass_on(s - 1)

        return carry

    lax.fori_loop(1, h + 2, back, 0)

    own = (h - 1) * 2 + 1
    for sub in range(2):
        rows = slice(sub * HALF, sub * HALF + HALF)
        total = mixed_ref[rows, :] + keep[own, rows, :] + prs[own, rows, :].astype(F32)
        for direction in range(2):
            slot_of = (direction * 2 + sub) * h + h - 1
            wait_bytes(rsr.at[slot_of], rs_recv.at[slot_of])
            total = total + rsr[slot_of].astype(F32)
        out_ref[rows, :] = total.astype(BF16)

    ring.finish()
    wait_bytes(ret.at[pl.ds(0, h * (ntp - 1))], disp_send)
    wait_bytes(ret.at[pl.ds(0, h * (ntp - 1))], ret_send)
    wait_bytes(prs, pair_send)
    wait_bytes(rsr.at[pl.ds(0, 4 * h - 2)], rs_send)


def local(dims, q, k, v, q_gain, k_gain, residual, out_weight, route_expert, route_weight, gate, up, down):
    nz, ny, nx = dims
    ntp = ny * nx
    h = nz // 2
    width = ntp * LANES
    experts = ntp // 2
    vmem = pl.BlockSpec(memory_space=pltpu.VMEM)
    hbm = pl.BlockSpec(memory_space=pl.ANY)
    dma = pltpu.SemaphoreType.DMA
    route = jnp.concatenate([route_expert.astype(F32).T, route_weight.T], axis=0)
    rowtab, coltab = rotation_constants(nz * 8)
    mixed, routes = pl.pallas_call(
        functools.partial(attention_kernel, dims),
        out_shape=(
            jax.ShapeDtypeStruct((TOK, LANES), F32),
            jax.ShapeDtypeStruct((2 * nz, 16, TOK), F32),
        ),
        in_specs=[vmem] * 10,
        out_specs=(vmem, vmem),
        scratch_shapes=[
            pltpu.VMEM((2 * nz, TOK, LANES), BF16),
            pltpu.VMEM((2 * nz, 16, TOK), F32),
            pltpu.VMEM((2 * TOK, LANES), BF16),
            pltpu.VMEM((1, 2 * TOK), F32),
            pltpu.VMEM((1, 2 * TOK), F32),
            pltpu.VMEM((LANES, 2 * TOK), F32),
            pltpu.VMEM((TOK, LANES), BF16),
            pltpu.VMEM((TOK, width), BF16),
            dma, dma((2, 2, h + 1)), dma((2 * h, 2)),
            dma, dma((2, h + 1)), dma((2 * h,)),
            dma, dma,
        ],
        compiler_params=pltpu.CompilerParams(
            collective_id=0, has_side_effects=True, vmem_limit_bytes=40 * 1024 * 1024
        ),
        name="attend",
    )(q, k, v, q_gain, k_gain, residual, out_weight, route, jnp.asarray(rowtab), jnp.asarray(coltab))
    rows = h * GROUP
    return pl.pallas_call(
        functools.partial(expert_kernel, dims),
        out_shape=jax.ShapeDtypeStruct((TOK, LANES), BF16),
        in_specs=[vmem, vmem, hbm, hbm, hbm],
        out_specs=vmem,
        scratch_shapes=[
            pltpu.VMEM((2 * nz, TOK, LANES), BF16),
            pltpu.VMEM((2 * nz, 8, TOK), F32),
            pltpu.VMEM((2 * nz, 8, TOK), F32),
            pltpu.VMEM((2 * nz, 8, TOK), F32),
            pltpu.VMEM((h, experts * GROUP, 4 * TOK), BF16),
            pltpu.VMEM((h, GROUP, LANES), F32),
            pltpu.VMEM((h, experts, GROUP, LANES), BF16),
            pltpu.VMEM((rows, width), BF16),
            pltpu.VMEM((width, 256), BF16),
            pltpu.VMEM((width, 256), BF16),
            pltpu.VMEM((256, width), BF16),
            pltpu.VMEM((ntp, h, GROUP, LANES), BF16),
            pltpu.VMEM((h * ntp, GROUP, LANES), BF16),
            pltpu.VMEM((2 * h, TOK, LANES), F32),
            pltpu.VMEM((2 * h, TOK, LANES), BF16),
            pltpu.VMEM((2 * h, TOK, LANES), BF16),
            pltpu.VMEM((4 * h, HALF, LANES), BF16),
            pltpu.VMEM((4 * h, HALF, LANES), BF16),
            dma, dma((2, 2, h + 1)), dma((2 * h, 2)),
            dma, dma((h,)), dma((h,)), dma((3,)),
            dma, dma((h,)), dma((h,)),
            dma, dma((2 * h,)), dma, dma((4 * h,)),
        ],
        compiler_params=pltpu.CompilerParams(
            collective_id=1, has_side_effects=True, vmem_limit_bytes=60 * 1024 * 1024
        ),
        name="experts",
    )(mixed, routes, gate, up, down)


def build(devices, dims):
    nz, ny, nx = dims
    split = Mesh(devices.reshape(nz, 2, ny, nx), ALL)
    in_specs = (
        P(SP, TP), P(SP, TP), P(SP, TP), P(TP, None), P(TP, None), P(SP, TP), P(None, TP),
        P(SP, None), P(SP, None), P(ALL, None, None), P(ALL, None, None), P(ALL, None, None),
    )
    return jax.shard_map(
        functools.partial(local, dims), mesh=split, in_specs=in_specs,
        out_specs=P(SP, TP), check_vma=False,
    )


def solution(mesh):
    return build(mesh.devices, (mesh.shape["sp"] // 2, 4, mesh.shape["tp"] // 4))
```
